32 devices in a mesh: ep: 8 (over z, y), tp: 4 (over x, core).
Axes of the slice: x: 2, y: 2, z: 4, core: 2. Of those that a mesh axis runs over, the one named last changes fastest.
Arguments:
- outer_gate: bfloat16 [4096, 2048], P('ep', 'tp'), may hold values from -6 to 6
- inner_gate: bfloat16 [4096, 2048], P('ep', 'tp'), may hold values from -6 to 6
- conv_values: bfloat16 [4096, 2048], P('ep', 'tp'), may hold values from -6 to 6
- conv_taps: bfloat16 [3, 2048], P(None, 'tp'), may hold values from -3 to 3
- out_weight: bfloat16 [2048, 2048], P('tp'), may hold values from -0.125 to 0.125
- moe_input: bfloat16 [4096, 2048], P(('ep', 'tp')), may hold values from -6 to 6
- norm_gain: bfloat16 [2048], replicated, may hold values from 0.099609375 to 1.8984375
- gate_proj: bfloat16 [8, 2048, 1024], P('ep', None, 'tp'), may hold values from -0.125 to 0.125
- up_proj: bfloat16 [8, 2048, 1024], P('ep', None, 'tp'), may hold values from -0.125 to 0.125
- down_proj: bfloat16 [8, 1024, 2048], P('ep', 'tp'), may hold values from -0.1875 to 0.1875
- shared_gate: bfloat16 [2048, 1024], P(None, 'tp'), may hold values from -0.125 to 0.125
- shared_up: bfloat16 [2048, 1024], P(None, 'tp'), may hold values from -0.125 to 0.125
- shared_down: bfloat16 [1024, 2048], P('tp'), may hold values from -0.1875 to 0.1875
- routes: int32 [4096, 2], P('ep'), may hold values from 0 to 7, all different within a row; in each aligned block of 128 rows (0 to 127, 128 to 255, ...) at most 64 rows name the same one
- route_weight: float32 [4096, 2], P('ep'), may hold values from 0.3 to 1.5
Outputs:
- mixer_out: bfloat16 [4096, 2048], P(('ep', 'tp'))
- expert_mix: bfloat16 [4096, 2048], P(('ep', 'tp'))
The draws below stay inside these ranges and needn't reach their ends.
Inputs may be any that keep to these rules, and one draw needn't show every extreme that they name: `routes`: each row names 2 different experts. In the 128 rows of one device no expert is named more than 64 times, and in every draw some expert is named exactly 64 times in one device's rows.
All inputs are finite; a program needn't handle non-finite values.
Results may differ from the reference program's by a relative error of at most 0.012.
Values may be sent and summed in bfloat16 or wider, within the bound.
A program may use at most 128 MiB of HBM per device.

```python
import math
import jax
import jax.numpy as jnp
import numpy as np
from jax import lax

D = 2048
EH = 1024
SH = 1024
TOPK = 2
TAPS = 3
R2 = 128
EXPERTS = 8
CAP = 64
TOK1 = 4096
TOK2 = 4096
N_EP = 8
N_TP = 4


def block_scale(rng, dims, cuts, low, top_value):
    gain = 1.0
    for position, blocks in cuts:
        draws = jax.random.uniform(jax.random.fold_in(jax.random.fold_in(rng, 6), position), (blocks,), jnp.float32, low / len(cuts), top_value / len(cuts))
        gain = gain * jnp.repeat(jnp.exp(draws), dims[position] // blocks).reshape((-1,) + (1,) * (len(dims) - 1 - position))
    return gain


def assign_block(key, own, number, rows, number_of, top, limit, skew):
    ranking = jax.random.permutation(key, number_of)
    heavy_load, common = shares(number_of, rows * top, limit, skew, True), shares(number_of, rows * top, limit, skew, False)
    places = jnp.arange(number_of)

    def named(tallies, turn):
        used = int((tallies > 0).sum())
        fixed = max(1, used // 4)
        passed = fixed + (places - fixed + turn * (used - fixed)) % max(1, number_of - fixed)
        return jnp.zeros((number_of,), jnp.int32).at[ranking[jnp.where(places < fixed, places, passed)]].set(jnp.asarray(tallies, jnp.int32))

    tallies = jnp.where(number % 4 == 0, named(heavy_load, number // 4), named(common, number - number // 4 - 1))
    mixed = jax.random.permutation(jax.random.fold_in(own, 3), number_of)
    donor, receiver = mixed[0:number_of // 2 * 2:2], mixed[1:number_of // 2 * 2:2]
    room = jnp.minimum(tallies[donor] - 1, limit - tallies[receiver]) // 2
    room = jnp.where((donor == ranking[0]) | (receiver == ranking[0]) | (tallies[receiver] == 0), 0, jnp.maximum(room, 0))
    passed = jax.random.randint(jax.random.fold_in(own, 4), (number_of // 2,), 0, 1 << 20) % (room + 1)
    tallies = tallies.at[donor].add(-passed).at[receiver].add(passed)
    items = jnp.searchsorted(jnp.cumsum(tallies), jnp.arange(rows * top), side="right").astype(jnp.int32)
    table = items.reshape(top, rows).T
    table = table[jax.random.permutation(jax.random.fold_in(own, 1), rows)]
    turn = jax.random.randint(jax.random.fold_in(own, 2), (rows, 1), 0, top)
    return jnp.take_along_axis(table, (jnp.arange(top)[None, :] + turn) % top, axis=1)


def shares(count, total, bound, slope, full):
    weights = [(1 << 20) // math.isqrt(standing ** slope) + 1 for standing in range(1, count + 1)]
    largest = bound if full else min(bound, max(-(-total // count), total * weights[0] // sum(weights)))
    least = 1 if total - largest >= count - 1 else 0
    given, surplus = [largest] + [least] * (count - 1), total - largest - least * (count - 1)
    while surplus > 0:
        movable = [i for i in range(1, count) if given[i] < largest] or [i for i in range(1, count) if given[i] < bound]
        pool, budget = sum([weights[i] for i in movable]), surplus
        for i in movable:
            extra = min(bound - given[i], max(1, budget * weights[i] // pool), surplus)
            given[i] = given[i] + extra
            surplus = surplus - extra
    return np.array(given)


def normal_values(key, shape, spread, bound, split=(), held_as=jnp.bfloat16):
    drawn = jax.random.normal(key, shape, jnp.float32) * spread
    if len(split) > 0:
        drawn = block_scale(key, shape, split, -0.22, 0.18) * drawn
    return jnp.clip(drawn, min=-bound, max=bound).astype(held_as)


def setup_inputs(seed: int = 0) -> dict:
    key_of = jax.random.split(jax.random.key(seed), 16)
    outer_gate = normal_values(key_of[0], (TOK1, D), 1.0, 6.0, ((0, 8), (1, 4)))
    inner_gate = normal_values(key_of[1], (TOK1, D), 1.0, 6.0, ((0, 8), (1, 4)))
    conv_values = normal_values(key_of[2], (TOK1, D), 1.0, 6.0, ((0, 8), (1, 4)))
    conv_taps = normal_values(key_of[3], (TAPS, D), 0.577, 3.0, ((1, 4),))
    out_weight = normal_values(key_of[4], (D, D), D ** -0.5, 0.125, ((0, 4),))
    moe_input = normal_values(key_of[5], (TOK2, D), 1.0, 6.0, ((0, 32),))
    norm_gain = jnp.clip(1.0 + 0.18 * jax.random.normal(key_of[6], (D,), jnp.float32), 0.099609375, 1.8984375).astype(jnp.bfloat16)
    gate_proj = normal_values(key_of[7], (EXPERTS, D, EH), D ** -0.5, 0.125, ((0, 8), (2, 4)))
    up_proj = normal_values(key_of[8], (EXPERTS, D, EH), D ** -0.5, 0.125, ((0, 8), (2, 4)))
    down_proj = normal_values(key_of[9], (EXPERTS, EH, D), EH ** -0.5, 0.1875, ((0, 8), (1, 4)))
    shared_gate = normal_values(key_of[10], (D, SH), D ** -0.5, 0.125, ((1, 4),))
    shared_up = normal_values(key_of[11], (D, SH), D ** -0.5, 0.125, ((1, 4),))
    shared_down = normal_values(key_of[12], (SH, D), SH ** -0.5, 0.1875, ((0, 4),))
    routes_keys = jax.random.split(jax.random.fold_in(key_of[13], 1), TOK2 // R2)
    routes_turns = jax.random.permutation(jax.random.fold_in(key_of[13], 3), TOK2 // R2)
    routes = jax.vmap(lambda own, number: assign_block(jax.random.fold_in(key_of[13], 2), own, number, R2, N_EP, TOPK, CAP, 2))(routes_keys, routes_turns).reshape((TOK2, TOPK))
    route_weight = jnp.clip(0.3 + 1.2 * jax.random.uniform(key_of[14], (TOK2, TOPK), jnp.float32) ** block_scale(key_of[14], (TOK2, TOPK), ((0, 8),), -0.2, 0.2), 0.3, 1.5)
    return dict(outer_gate=outer_gate, inner_gate=inner_gate, conv_values=conv_values, conv_taps=conv_taps, out_weight=out_weight, moe_input=moe_input, norm_gain=norm_gain, gate_proj=gate_proj, up_proj=up_proj, down_proj=down_proj, shared_gate=shared_gate, shared_up=shared_up, shared_down=shared_down, routes=routes, route_weight=route_weight)


epsilon = 1e-06

def rms_norm(inputs, scales):
    values = inputs.astype(jnp.float32)
    square = lax.optimization_barrier(jnp.mean(values * values, axis=-1, keepdims=True))
    return (values * lax.rsqrt(square + epsilon) * scales.astype(jnp.float32)).astype(jnp.bfloat16)

def summed_parts(hidden, weight, pieces):
    stride = hidden.shape[1] // pieces
    result = jnp.zeros((hidden.shape[0], weight.shape[1]), jnp.float32)
    for piece_idx in range(pieces):
        partial_sum = jnp.dot(hidden[:, piece_idx * stride:(piece_idx + 1) * stride], weight[piece_idx * stride:(piece_idx + 1) * stride], preferred_element_type=jnp.float32).astype(jnp.bfloat16)
        partial_sum = lax.optimization_barrier(partial_sum)
        result = result + partial_sum.astype(jnp.float32)
    return result

def swiglu(inputs, gate_w, up_w):
    gate_term = jnp.dot(inputs, gate_w, preferred_element_type=jnp.float32)
    upward = jnp.dot(inputs, up_w, preferred_element_type=jnp.float32)
    return (jax.nn.silu(gate_term) * upward).astype(jnp.bfloat16)

def reference(outer_gate, inner_gate, conv_values, conv_taps, out_weight, moe_input, norm_gain, gate_proj, up_proj, down_proj, shared_gate, shared_up, shared_down, routes, route_weight):
    product = inner_gate.astype(jnp.float32) * conv_values.astype(jnp.float32)
    length = product.shape[0]
    padded = jnp.pad(product, ((TAPS - 1, 0), (0, 0)))
    tap_values = conv_taps.astype(jnp.float32)
    convolved = jnp.zeros_like(product)
    for offset in range(TAPS):
        convolved = convolved + tap_values[offset] * padded[offset:offset + length]
    gate_rows = (outer_gate.astype(jnp.float32) * convolved).astype(jnp.bfloat16)
    mixer_out = summed_parts(gate_rows, out_weight, N_TP).astype(jnp.bfloat16)
    normed = rms_norm(moe_input, norm_gain)
    tokens = normed.shape[0]
    slot_limit = N_EP * N_TP * CAP
    token_ids = jnp.arange(tokens, dtype=jnp.int32)

    def one_expert(running, operands):
        expert, gate_w, up_w, down_w = operands
        expert_hits = routes == expert
        chosen = jnp.any(expert_hits, axis=1)
        weight_sum = lax.optimization_barrier(jnp.sum(jnp.where(expert_hits, route_weight, jnp.float32(0.0)), axis=1))
        places = jnp.cumsum(chosen.astype(jnp.int32)) - 1
        targets = jnp.where(chosen, places, slot_limit).astype(jnp.int32)
        row_table = jnp.zeros((slot_limit,), jnp.int32).at[targets].set(token_ids, mode='drop')
        filled = jnp.zeros((slot_limit,), jnp.float32).at[targets].set(1.0, mode='drop')
        hidden = swiglu(normed[row_table], gate_w, up_w)
        result = summed_parts(hidden, down_w, N_TP).astype(jnp.bfloat16)
        result = lax.optimization_barrier(result)
        scaled = result.astype(jnp.float32) * (weight_sum[row_table] * filled)[:, None]
        return (running.at[row_table].add(scaled), None)
    routed, _ = lax.scan(one_expert, jnp.zeros((tokens, normed.shape[1]), jnp.float32), (jnp.arange(N_EP, dtype=jnp.int32), gate_proj, up_proj, down_proj))
    shared_hidden = swiglu(normed, shared_gate, shared_up)
    shared_sum = summed_parts(shared_hidden, shared_down, N_TP)
    expert_mix = (shared_sum + routed).astype(jnp.bfloat16)
    return (mixer_out, expert_mix)
```

```python
import functools

import jax
import jax.numpy as jnp
from jax import lax
from jax.experimental import pallas as pl
from jax.experimental.pallas import tpu as pltpu
from jax.sharding import PartitionSpec as P

epsilon = 1e-06
MESH = pl.DeviceIdType.MESH
f32 = jnp.float32
bf16 = jnp.bfloat16
CHUNKS = 4


def dot(a, b):
    return jnp.dot(a, b, preferred_element_type=f32)


def kernel(
    dims,
    outer, inner, values, taps, out_w, tokens, gain, gate_p, up_p, down_p,
    sh_gate, sh_up, sh_down, routes, weights,
    mix_o, exp_o,
    l_outer, l_inner, l_values, halo, prod, l_out_w, l_sg, l_su, l_sd,
    gf, uf, df, nf, og, ld, hid, rt, rv,
    parts, pairs, sums, arrived,
    loc_sem, halo_send, halo_recv, x_send, p_send, t_recv,
    d_send, d_recv, b_send, b_recv, r_send, r_recv, rx_send, rx_recv,
):
    ep, tp, cap = dims
    half = tp // 2
    e, t = lax.axis_index("ep"), lax.axis_index("tp")
    a, b = t // 2, lax.rem(t, 2)
    pair = (e, 2 * a + 1 - b)
    group, ch = l_inner.shape
    rows, width = tokens.shape
    slots = ep * cap
    cols = width // CHUNKS
    n_taps = taps.shape[0]

    def far(d):
        return 2 * lax.rem(a + d, half) + b

    def near(d):
        return 2 * lax.rem(a + half - d, half) + b

    def remote(src, dst, s, r, dev):
        return pltpu.make_async_remote_copy(
            src_ref=src, dst_ref=dst, send_sem=s, recv_sem=r, device_id=dev, device_id_type=MESH
        )

    barrier = pltpu.get_barrier_semaphore()

    def greet(d, _):
        pl.semaphore_signal(barrier, inc=1, device_id=(lax.rem(e + d, ep), t), device_id_type=MESH)
        return 0

    lax.fori_loop(1, ep, greet, 0)
    pl.semaphore_signal(barrier, inc=1, device_id=pair, device_id_type=MESH)
    for d in range(1, half):
        pl.semaphore_signal(barrier, inc=1, device_id=(e, far(d)), device_id_type=MESH)

    local = [
        pltpu.make_async_copy(s, d, loc_sem.at[i])
        for i, (s, d) in enumerate(
            (
                (inner, l_inner), (values, l_values), (outer, l_outer), (out_w, l_out_w),
                (sh_gate, l_sg), (sh_up, l_su), (sh_down, l_sd),
                (gate_p.at[0], gf.at[t]), (up_p.at[0], uf.at[t]), (down_p.at[0], df.at[t]),
            )
        )
    ]
    for c in local:
        c.start()

    def norm_rows(i, _):
        at = pl.ds(pl.multiple_of(i * 16, 16), 16)
        v = tokens[at, :].astype(f32)
        square = jnp.mean(v * v, axis=-1, keepdims=True)
        nf[t, at, :] = (v * lax.rsqrt(square + epsilon) * gain[...].astype(f32)).astype(bf16)
        return 0

    lax.fori_loop(0, rows // 16, norm_rows, 0)
    mine = pl.ds(pl.multiple_of(t * rows, rows), rows)
    own_routes, own_w = routes[mine, :], weights[mine, :]
    slot = lax.broadcasted_iota(jnp.int32, (rows, slots), 1)
    expert = slot // cap
    place = (slot - expert * cap).astype(f32)
    hit = jnp.zeros((rows, slots), f32)
    scale = jnp.zeros((rows, slots), f32)
    for k in range(own_routes.shape[1]):
        same = own_routes[:, k : k + 1] == expert
        hit = jnp.where(same, 1.0, hit)
        scale = jnp.where(same, own_w[:, k : k + 1], scale)
    lower = lax.broadcasted_iota(jnp.int32, (rows, rows), 0) > lax.broadcasted_iota(
        jnp.int32, (rows, rows), 1
    )
    earlier = dot(jnp.where(lower, 1.0, 0.0).astype(bf16), hit.astype(bf16))
    chosen = jnp.where(earlier == place, hit, 0.0)
    w_all = chosen * scale
    w_hi = w_all.astype(bf16)
    w_lo = (w_all - w_hi.astype(f32)).astype(bf16)
    sender = jnp.transpose(chosen).astype(bf16)

    pl.semaphore_wait(barrier, ep - 1 + 1 + half - 1)

    kinds = CHUNKS + 3
    n_kind = kinds - 1

    def land(k, s):
        if k == 0:
            return gf.at[s]
        if k == 1:
            return uf.at[s]
        if k == n_kind:
            return nf.at[s]
        return df.at[s, :, pl.ds((k - 2) * cols, cols)]

    def origin(k):
        if k == 0:
            return gate_p.at[0]
        if k == 1:
            return up_p.at[0]
        if k == n_kind:
            return nf.at[t]
        return down_p.at[0, :, pl.ds((k - 2) * cols, cols)]

    def x_copy(k, d):
        return remote(origin(k), land(k, t), x_send.at[k, d], t_recv.at[k, d], (e, far(d)))

    def pair_copy(k):
        return remote(origin(k), land(k, t), p_send.at[k, 0], t_recv.at[k, 0], pair)

    def forward_copy(k, d):
        s = near(d)
        return remote(land(k, s), land(k, s), p_send.at[k, d], t_recv.at[k, half - 1 + d], pair)

    def start_x(k):
        for d in range(1, half):
            x_copy(k, d).start()

    def forward(k):
        for d in range(1, half):
            x_copy(k, d).wait_recv()
            forward_copy(k, d).start()

    def wait_forwarded(k):
        for d in range(1, half):
            forward_copy(k, d).wait_recv()

    start_x(0)
    start_x(1)
    edge = pl.ds(group - 16, 16)
    halos = [
        remote(src.at[edge, :], halo.at[i], halo_send.at[i], halo_recv.at[i], (lax.rem(e + 1, ep), t))
        for i, src in enumerate((inner, values))
    ]
    for c in halos:
        c.start()

    def block(i):
        return pl.ds(pl.multiple_of(i * cap, cap), cap)

    def dispatch_copy(d):
        to = lax.rem(e + d, ep)
        return remote(og.at[block(to), :], ld.at[block(e), :], d_send.at[d], d_recv.at[d], (to, t))

    for c in range(CHUNKS):
        at = pl.ds(c * cols, cols)
        og[:, at] = dot(sender, nf[t, :, at]).astype(bf16)

    def start_dispatch(d, _):
        dispatch_copy(d).start()
        return 0

    lax.fori_loop(1, ep, start_dispatch, 0)
    ld[block(e), :] = og[block(e), :]
    for k in range(kinds):
        pair_copy(k).start()
    for k in range(2, kinds):
        start_x(k)

    def pair_sum(j, i):
        return remote(
            parts.at[j, 2 * i + 1 - b], pairs.at[j, i], r_send.at[j, i], r_recv.at[j, i], pair
        )

    def far_sum(j, d):
        return remote(
            sums.at[j, d - 1], arrived.at[j, d - 1], rx_send.at[j, d], rx_recv.at[j, d], (e, far(d))
        )

    def start_far(j):
        for d in range(1, half):
            i = lax.rem(a + d, half)
            pair_sum(j, i).wait_recv()
            for c in range(CHUNKS):
                at = pl.ds(c * cols, cols)
                total = parts[j, 2 * i + b, :, at].astype(f32) + pairs[j, i, :, at].astype(f32)
                sums[j, d - 1, :, at] = total.astype(bf16)
            far_sum(j, d).start()

    def finish_sum(j):
        pair_sum(j, a).wait_recv()
        for d in range(1, half):
            far_sum(j, d).wait_recv()

    def summed(j, at):
        total = parts[j, t, :, at].astype(f32) + pairs[j, a, :, at].astype(f32)
        for d in range(1, half):
            total = total + arrived[j, d - 1, :, at].astype(f32)
        return total

    for c in local[:4]:
        c.wait()
    for c in halos:
        c.wait_recv()
    before = halo[0].astype(f32) * halo[1].astype(f32)
    prod[0:16, :] = jnp.where(e > 0, before, 0.0)
    prod[16:, :] = l_inner[...].astype(f32) * l_values[...].astype(f32)
    tap = taps[...].astype(f32)
    for s in range(tp):
        lo = s * rows
        conv = jnp.zeros((rows, ch), f32)
        for j in range(n_taps):
            first = 16 + lo - (n_taps - 1) + j
            conv = conv + tap[j : j + 1, :] * prod[first : first + rows, :]
        gated = (l_outer[lo : lo + rows, :].astype(f32) * conv).astype(bf16)
        for c in range(CHUNKS):
            at = pl.ds(c * cols, cols)
            parts[0, s, :, at] = dot(gated, l_out_w[:, at]).astype(bf16)
    for i in range(half):
        pair_sum(0, i).start()

    for c in local[4:]:
        c.wait()

    def shared(s):
        x = nf[s]
        g = dot(x, l_sg[...])
        u = dot(x, l_su[...])
        h = (g / (1.0 + jnp.exp(-g)) * u).astype(bf16)
        for c in range(CHUNKS):
            at = pl.ds(c * cols, cols)
            parts[1, s, :, at] = dot(h, l_sd[:, at]).astype(bf16)

    shared(t)
    start_far(0)
    pair_copy(n_kind).wait_recv()
    shared(2 * a + 1 - b)
    pair_sum(1, a).start()

    def wait_dispatch(d, _):
        dispatch_copy(d).wait_recv()
        return 0

    lax.fori_loop(1, ep, wait_dispatch, 0)

    def hidden(s):
        g = dot(ld[...], gf[s])
        u = dot(ld[...], uf[s])
        hid[s] = (g / (1.0 + jnp.exp(-g)) * u).astype(bf16)

    hidden(t)
    pair_copy(0).wait_recv()
    pair_copy(1).wait_recv()
    hidden(2 * a + 1 - b)
    forward(0)
    forward(1)
    for d in range(1, half):
        hidden(near(d))
    wait_forwarded(0)
    wait_forwarded(1)
    for d in range(1, half):
        hidden(near(d) + 1 - 2 * b)

    def back_copy(c, d):
        to = lax.rem(e + d, ep)
        at = pl.ds(c * cols, cols)
        return remote(
            rt.at[block(to), at], rv.at[block(e), at], b_send.at[c, d], b_recv.at[c, d], (to, t)
        )

    for c in range(CHUNKS):
        k = 2 + c
        at = pl.ds(c * cols, cols)
        pair_copy(k).wait_recv()
        forward(k)
        wait_forwarded(k)
        total = dot(hid[0], df[0, :, at])
        for s in range(1, tp):
            total = total + dot(hid[s], df[s, :, at])
        rt[:, at] = total.astype(bf16)

        def start_back(d, _):
            back_copy(c, d).start()
            return 0

        lax.fori_loop(1, ep, start_back, 0)
        rv[block(e), at] = rt[block(e), at]

    forward(n_kind)
    for d in range(1, half):
        shared(near(d))
    wait_forwarded(n_kind)
    for d in range(1, half):
        shared(near(d) + 1 - 2 * b)
        pair_sum(1, lax.rem(a + half - d, half)).start()
    start_far(1)

    finish_sum(0)
    for c in range(CHUNKS):
        at = pl.ds(c * cols, cols)
        mix_o[:, at] = summed(0, at).astype(bf16)
    finish_sum(1)
    for c in range(CHUNKS):
        at = pl.ds(c * cols, cols)

        def wait_back(d, _):
            back_copy(c, d).wait_recv()
            return 0

        lax.fori_loop(1, ep, wait_back, 0)
        routed = dot(w_hi, rv[:, at]) + dot(w_lo, rv[:, at])
        exp_o[:, at] = (summed(1, at) + routed).astype(bf16)

    def sent(d, _):
        dispatch_copy(d).wait_send()
        for c in range(CHUNKS):
            back_copy(c, d).wait_send()
        return 0

    lax.fori_loop(1, ep, sent, 0)
    for c in halos:
        c.wait_send()
    for k in range(kinds):
        pair_copy(k).wait_send()
        for d in range(1, half):
            x_copy(k, d).wait_send()
            forward_copy(k, d).wait_send()
    for j in range(2):
        for i in range(half):
            pair_sum(j, i).wait_send()
        for d in range(1, half):
            far_sum(j, d).wait_send()


def per_device(
    outer_gate, inner_gate, conv_values, conv_taps, out_weight, moe_input, norm_gain,
    gate_proj, up_proj, down_proj, shared_gate, shared_up, shared_down, routes, route_weight,
):
    tp = lax.axis_size("tp")
    ep = lax.axis_size("ep")
    half = tp // 2
    group, ch = inner_gate.shape
    rows, width = moe_input.shape
    units = gate_proj.shape[2]
    sh_units = shared_gate.shape[1]
    cap = 2 * rows * routes.shape[1] // ep
    cap = -(-cap // 16) * 16
    slots = ep * cap
    kinds = CHUNKS + 3
    any_spec = pl.BlockSpec(memory_space=pl.ANY)
    vmem = pl.BlockSpec(memory_space=pltpu.VMEM)
    dma = pltpu.SemaphoreType.DMA

    def buf(*shape):
        return pltpu.VMEM(shape, bf16)

    scratch = [
        buf(group, ch), buf(group, ch), buf(group, ch), buf(2, 16, ch),
        pltpu.VMEM((group + 16, ch), f32), buf(ch, width),
        buf(width, sh_units), buf(width, sh_units), buf(sh_units, width),
        buf(tp, width, units), buf(tp, width, units), buf(tp, units, width),
        buf(tp, rows, width), buf(slots, width), buf(slots, width),
        buf(tp, slots, units), buf(slots, width), buf(slots, width),
        buf(2, tp, rows, width), buf(2, half, rows, width),
        buf(2, half - 1, rows, width), buf(2, half - 1, rows, width),
        dma((10,)), dma((2,)), dma((2,)), dma((kinds, half)), dma((kinds, half)),
        dma((kinds, tp)), dma((ep,)), dma((ep,)), dma((CHUNKS, ep)), dma((CHUNKS, ep)),
        dma((2, half)), dma((2, half)), dma((2, half)), dma((2, half)),
    ]
    out = jax.ShapeDtypeStruct((rows, width), bf16)
    return pl.pallas_call(
        functools.partial(kernel, (ep, tp, cap)),
        out_shape=(out, out),
        in_specs=[
            any_spec, any_spec, any_spec, vmem, any_spec, vmem, vmem,
            any_spec, any_spec, any_spec, any_spec, any_spec, any_spec, vmem, vmem,
        ],
        out_specs=(vmem, vmem),
        scratch_shapes=scratch,
        compiler_params=pltpu.CompilerParams(
            collective_id=0, has_side_effects=True, vmem_limit_bytes=67043328
        ),
    )(
        outer_gate, inner_gate, conv_values, conv_taps, out_weight, moe_input,
        norm_gain.reshape(1, width), gate_proj, up_proj, down_proj,
        shared_gate, shared_up, shared_down, routes, route_weight,
    )


def solution(mesh):
    return jax.shard_map(
        per_device,
        mesh=mesh,
        in_specs=(
            P("ep", "tp"), P("ep", "tp"), P("ep", "tp"), P(None, "tp"), P("tp", None),
            P(("ep", "tp"), None), P(),
            P("ep", None, "tp"), P("ep", None, "tp"), P("ep", "tp", None),
            P(None, "tp"), P(None, "tp"), P("tp", None), P("ep", None), P("ep", None),
        ),
        out_specs=(P(("ep", "tp"), None), P(("ep", "tp"), None)),
        check_vma=False,
    )
```

```python
import functools

import jax
import jax.numpy as jnp
from jax import lax
from jax.experimental import pallas as pl
from jax.experimental.pallas import tpu as pltpu
from jax.sharding import PartitionSpec as P

epsilon = 1e-06
MESH = pl.DeviceIdType.MESH
f32 = jnp.float32
bf16 = jnp.bfloat16
CHUNKS = 4


def dot(a, b):
    return jnp.dot(a, b, preferred_element_type=f32)


def kernel(
    dims,
    outer, inner, values, taps, out_w, tokens, gain, gate_p, up_p, down_p,
    sh_gate, sh_up, sh_down, routes, weights,
    mix_o, exp_o,
    l_outer, l_inner, l_values, halo, prod, l_out_w, l_sg, l_su, l_sd,
    gf, uf, df, nf, og, ld, hid, rt, rv,
    acc, parts, pairs, sums, arrived,
    loc_sem, halo_send, halo_recv, x_send, p_send, t_recv,
    d_send, d_recv, b_send, b_recv, r_send, r_recv, rx_send, rx_recv,
):
    ep, tp, cap = dims
    half = tp // 2
    e, t = lax.axis_index("ep"), lax.axis_index("tp")
    a, b = t // 2, lax.rem(t, 2)
    pair = (e, 2 * a + 1 - b)
    group, ch = l_inner.shape
    rows, width = tokens.shape
    slots = ep * cap
    cols = width // CHUNKS
    n_taps = taps.shape[0]

    def far(d):
        return 2 * lax.rem(a + d, half) + b

    def near(d):
        return 2 * lax.rem(a + half - d, half) + b

    def remote(src, dst, s, r, dev):
        return pltpu.make_async_remote_copy(
            src_ref=src, dst_ref=dst, send_sem=s, recv_sem=r, device_id=dev, device_id_type=MESH
        )

    barrier = pltpu.get_barrier_semaphore()

    def greet(d, _):
        pl.semaphore_signal(barrier, inc=1, device_id=(lax.rem(e + d, ep), t), device_id_type=MESH)
        return 0

    lax.fori_loop(1, ep, greet, 0)
    pl.semaphore_signal(barrier, inc=1, device_id=pair, device_id_type=MESH)
    for d in range(1, half):
        pl.semaphore_signal(barrier, inc=1, device_id=(e, far(d)), device_id_type=MESH)

    local = [
        pltpu.make_async_copy(s, d, loc_sem.at[i])
        for i, (s, d) in enumerate(
            (
                (inner, l_inner), (values, l_values), (outer, l_outer), (out_w, l_out_w),
                (sh_gate, l_sg), (sh_up, l_su), (sh_down, l_sd),
                (gate_p.at[0], gf.at[t]), (up_p.at[0], uf.at[t]), (down_p.at[0], df.at[t]),
            )
        )
    ]
    for c in local:
        c.start()

    pl.semaphore_wait(barrier, ep - 1 + 1 + half - 1)

    kinds = CHUNKS + 3
    n_kind = kinds - 1

    def land(k, s):
        if k == 0:
            return gf.at[s]
        if k == 1:
            return uf.at[s]
        if k == n_kind:
            return nf.at[s]
        return df.at[s, :, pl.ds((k - 2) * cols, cols)]

    def origin(k):
        if k == 0:
            return gate_p.at[0]
        if k == 1:
            return up_p.at[0]
        if k == n_kind:
            return nf.at[t]
        return down_p.at[0, :, pl.ds((k - 2) * cols, cols)]

    def x_copy(k, d):
        return remote(origin(k), land(k, t), x_send.at[k, d], t_recv.at[k, d], (e, far(d)))

    def pair_copy(k):
        return remote(origin(k), land(k, t), p_send.at[k, 0], t_recv.at[k, 0], pair)

    def forward_copy(k, d):
        s = near(d)
        return remote(land(k, s), land(k, s), p_send.at[k, d], t_recv.at[k, half - 1 + d], pair)

    def start_x(k):
        for d in range(1, half):
            x_copy(k, d).start()

    def forward(k):
        for d in range(1, half):
            x_copy(k, d).wait_recv()
            forward_copy(k, d).start()

    def wait_forwarded(k):
        for d in range(1, half):
            forward_copy(k, d).wait_recv()

    for k in range(4):
        start_x(k)
    mine = pl.ds(pl.multiple_of(t * rows, rows), rows)
    own_routes, own_w = routes[:, mine], weights[:, mine]
    slot = lax.broadcasted_iota(jnp.int32, (slots, rows), 0)
    expert = slot // cap
    place = (slot - expert * cap).astype(f32)
    hit = jnp.zeros((slots, rows), f32)
    for k in range(own_routes.shape[0]):
        hit = jnp.where(own_routes[k : k + 1, :] == expert, 1.0, hit)
    upper = lax.broadcasted_iota(jnp.int32, (rows, rows), 0) < lax.broadcasted_iota(
        jnp.int32, (rows, rows), 1
    )
    earlier = dot(hit.astype(bf16), jnp.where(upper, 1.0, 0.0).astype(bf16))
    chosen = jnp.where(earlier == place, hit, 0.0)
    sender = chosen.astype(bf16)

    def norm_rows(i, _):
        at = pl.ds(pl.multiple_of(i * 16, 16), 16)
        v = tokens[at, :].astype(f32)
        square = jnp.mean(v * v, axis=-1, keepdims=True)
        nf[t, at, :] = (v * lax.rsqrt(square + epsilon) * gain[...].astype(f32)).astype(bf16)
        return 0

    lax.fori_loop(0, rows // 16, norm_rows, 0)

    def block(i):
        return pl.ds(pl.multiple_of(i * cap, cap), cap)

    def dispatch_copy(c, d):
        to = lax.rem(e + d, ep)
        at = pl.ds(c * cols, cols)
        return remote(
            og.at[block(to), at], ld.at[block(e), at], d_send.at[c, d], d_recv.at[c, d], (to, t)
        )

    for c in range(CHUNKS):
        at = pl.ds(c * cols, cols)
        og[:, at] = dot(sender, nf[t, :, at]).astype(bf16)

        def start_dispatch(d, _):
            dispatch_copy(c, d).start()
            return 0

        lax.fori_loop(1, ep, start_dispatch, 0)
        ld[block(e), at] = og[block(e), at]
    start_x(n_kind)
    for k in range(kinds):
        pair_copy(k).start()
    for k in range(4, n_kind):
        start_x(k)
    edge = pl.ds(group - 16, 16)
    halos = [
        remote(src.at[edge, :], halo.at[i], halo_send.at[i], halo_recv.at[i], (lax.rem(e + 1, ep), t))
        for i, src in enumerate((inner, values))
    ]
    for c in halos:
        c.start()


    def pair_sum(j, i):
        return remote(
            parts.at[j, 2 * i + 1 - b], pairs.at[j, i], r_send.at[j, i], r_recv.at[j, i], pair
        )

    def far_sum(j, d):
        return remote(
            sums.at[j, d - 1], arrived.at[j, d - 1], rx_send.at[j, d], rx_recv.at[j, d], (e, far(d))
        )

    def start_far(j):
        for d in range(1, half):
            i = lax.rem(a + d, half)
            pair_sum(j, i).wait_recv()
            for c in range(CHUNKS):
                at = pl.ds(c * cols, cols)
                total = parts[j, 2 * i + b, :, at].astype(f32) + pairs[j, i, :, at].astype(f32)
                sums[j, d - 1, :, at] = total.astype(bf16)
            far_sum(j, d).start()

    def finish_sum(j):
        pair_sum(j, a).wait_recv()
        for d in range(1, half):
            far_sum(j, d).wait_recv()

    def summed(j, at):
        total = parts[j, t, :, at].astype(f32) + pairs[j, a, :, at].astype(f32)
        for d in range(1, half):
            total = total + arrived[j, d - 1, :, at].astype(f32)
        return total

    for c in local[:4]:
        c.wait()
    for c in halos:
        c.wait_recv()
    before = halo[0].astype(f32) * halo[1].astype(f32)
    prod[0:16, :] = jnp.where(e > 0, before, 0.0)
    prod[16:, :] = l_inner[...].astype(f32) * l_values[...].astype(f32)
    tap = taps[...].astype(f32)
    for s in range(tp):
        lo = s * rows
        conv = jnp.zeros((rows, ch), f32)
        for j in range(n_taps):
            first = 16 + lo - (n_taps - 1) + j
            conv = conv + tap[j : j + 1, :] * prod[first : first + rows, :]
        gated = (l_outer[lo : lo + rows, :].astype(f32) * conv).astype(bf16)
        for c in range(CHUNKS):
            at = pl.ds(c * cols, cols)
            parts[0, s, :, at] = dot(gated, l_out_w[:, at]).astype(bf16)
    for i in range(half):
        pair_sum(0, i).start()

    for c in local[4:]:
        c.wait()

    def shared(s):
        x = nf[s]
        g = dot(x, l_sg[...])
        u = dot(x, l_su[...])
        h = (g / (1.0 + jnp.exp(-g)) * u).astype(bf16)
        for c in range(CHUNKS):
            at = pl.ds(c * cols, cols)
            parts[1, s, :, at] = dot(h, l_sd[:, at]).astype(bf16)

    shared(t)
    pair_copy(n_kind).wait_recv()
    shared(2 * a + 1 - b)
    pair_sum(1, a).start()

    def act(s, g, u):
        hid[s] = (g / (1.0 + jnp.exp(-g)) * u).astype(bf16)

    pair_copy(0).wait_recv()
    pair_copy(1).wait_recv()
    close = (t, 2 * a + 1 - b)
    for c in range(CHUNKS):
        at = pl.ds(c * cols, cols)

        def wait_dispatch(d, _):
            dispatch_copy(c, d).wait_recv()
            return 0

        lax.fori_loop(1, ep, wait_dispatch, 0)
        for i, s in enumerate(close):
            g, u = dot(ld[:, at], gf[s, at, :]), dot(ld[:, at], uf[s, at, :])
            if c:
                g, u = g + acc[i, 0], u + acc[i, 1]
            if c < CHUNKS - 1:
                acc[i, 0] = g
                acc[i, 1] = u
            else:
                act(s, g, u)
        if c == 1:
            forward(0)
    wait_forwarded(0)
    rest = [near(d) for d in range(1, half)] + [near(d) + 1 - 2 * b for d in range(1, half)]
    gates = [dot(ld[...], gf[s]) for s in rest]
    forward(1)
    for n, s in enumerate(rest):
        if n == half - 1:
            wait_forwarded(1)
        act(s, gates[n], dot(ld[...], uf[s]))

    def back_copy(c, d):
        to = lax.rem(e + d, ep)
        at = pl.ds(c * cols, cols)
        return remote(
            rt.at[block(to), at], rv.at[block(e), at], b_send.at[c, d], b_recv.at[c, d], (to, t)
        )

    for c in range(CHUNKS):
        k = 2 + c
        at = pl.ds(c * cols, cols)
        pair_copy(k).wait_recv()
        forward(k)
        wait_forwarded(k)
        total = dot(hid[0], df[0, :, at])
        for s in range(1, tp):
            total = total + dot(hid[s], df[s, :, at])
        rt[:, at] = total.astype(bf16)

        def start_back(d, _):
            back_copy(c, d).start()
            return 0

        lax.fori_loop(1, ep, start_back, 0)
        rv[block(e), at] = rt[block(e), at]
        if c == 1:
            forward(n_kind)
            for d in range(1, half):
                shared(near(d))
            wait_forwarded(n_kind)
            for d in range(1, half):
                shared(near(d) + 1 - 2 * b)
                pair_sum(1, lax.rem(a + half - d, half)).start()
            start_far(1)
            start_far(0)

    scale = jnp.zeros((slots, rows), f32)
    for k in range(own_routes.shape[0]):
        scale = jnp.where(own_routes[k : k + 1, :] == expert, own_w[k : k + 1, :], scale)
    w_all = jnp.transpose(chosen * scale)
    w_hi = w_all.astype(bf16)
    w_lo = (w_all - w_hi.astype(f32)).astype(bf16)
    finish_sum(1)
    for c in range(CHUNKS):
        at = pl.ds(c * cols, cols)

        def wait_back(d, _):
            back_copy(c, d).wait_recv()
            return 0

        lax.fori_loop(1, ep, wait_back, 0)
        routed = dot(w_hi, rv[:, at]) + dot(w_lo, rv[:, at])
        exp_o[:, at] = (summed(1, at) + routed).astype(bf16)

    finish_sum(0)
    for c in range(CHUNKS):
        at = pl.ds(c * cols, cols)
        mix_o[:, at] = summed(0, at).astype(bf16)
    def sent(d, _):
        for c in range(CHUNKS):
            dispatch_copy(c, d).wait_send()
            back_copy(c, d).wait_send()
        return 0

    lax.fori_loop(1, ep, sent, 0)
    for c in halos:
        c.wait_send()
    for k in range(kinds):
        pair_copy(k).wait_send()
        for d in range(1, half):
            x_copy(k, d).wait_send()
            forward_copy(k, d).wait_send()
    for j in range(2):
        for i in range(half):
            pair_sum(j, i).wait_send()
        for d in range(1, half):
            far_sum(j, d).wait_send()


def per_device(
    outer_gate, inner_gate, conv_values, conv_taps, out_weight, moe_input, norm_gain,
    gate_proj, up_proj, down_proj, shared_gate, shared_up, shared_down, routes, route_weight,
):
    tp = lax.axis_size("tp")
    ep = lax.axis_size("ep")
    half = tp // 2
    group, ch = inner_gate.shape
    rows, width = moe_input.shape
    units = gate_proj.shape[2]
    sh_units = shared_gate.shape[1]
    cap = 2 * rows * routes.shape[1] // ep
    cap = -(-cap // 16) * 16
    slots = ep * cap
    kinds = CHUNKS + 3
    any_spec = pl.BlockSpec(memory_space=pl.ANY)
    vmem = pl.BlockSpec(memory_space=pltpu.VMEM)
    dma = pltpu.SemaphoreType.DMA

    def buf(*shape):
        return pltpu.VMEM(shape, bf16)

    scratch = [
        buf(group, ch), buf(group, ch), buf(group, ch), buf(2, 16, ch),
        pltpu.VMEM((group + 16, ch), f32), buf(ch, width),
        buf(width, sh_units), buf(width, sh_units), buf(sh_units, width),
        buf(tp, width, units), buf(tp, width, units), buf(tp, units, width),
        buf(tp, rows, width), buf(slots, width), buf(slots, width),
        buf(tp, slots, units), buf(slots, width), buf(slots, width),
        pltpu.VMEM((2, 2, slots, units), f32), buf(2, tp, rows, width), buf(2, half, rows, width),
        buf(2, half - 1, rows, width), buf(2, half - 1, rows, width),
        dma((10,)), dma((2,)), dma((2,)), dma((kinds, half)), dma((kinds, half)),
        dma((kinds, tp)), dma((CHUNKS, ep)), dma((CHUNKS, ep)), dma((CHUNKS, ep)), dma((CHUNKS, ep)),
        dma((2, half)), dma((2, half)), dma((2, half)), dma((2, half)),
    ]
    out = jax.ShapeDtypeStruct((rows, width), bf16)
    return pl.pallas_call(
        functools.partial(kernel, (ep, tp, cap)),
        out_shape=(out, out),
        in_specs=[
            any_spec, any_spec, any_spec, vmem, any_spec, vmem, vmem,
            any_spec, any_spec, any_spec, any_spec, any_spec, any_spec, vmem, vmem,
        ],
        out_specs=(vmem, vmem),
        scratch_shapes=scratch,
        compiler_params=pltpu.CompilerParams(
            collective_id=0, has_side_effects=True, vmem_limit_bytes=67043328
        ),
    )(
        outer_gate, inner_gate, conv_values, conv_taps, out_weight, moe_input,
        norm_gain.reshape(1, width), gate_proj, up_proj, down_proj,
        shared_gate, shared_up, shared_down, routes.T, route_weight.T,
    )


def solution(mesh):
    return jax.shard_map(
        per_device,
        mesh=mesh,
        in_specs=(
            P("ep", "tp"), P("ep", "tp"), P("ep", "tp"), P(None, "tp"), P("tp", None),
            P(("ep", "tp"), None), P(),
            P("ep", None, "tp"), P("ep", None, "tp"), P("ep", "tp", None),
            P(None, "tp"), P(None, "tp"), P("tp", None), P("ep", None), P("ep", None),
        ),
        out_specs=(P(("ep", "tp"), None), P(("ep", "tp"), None)),
        check_vma=False,
    )
```

```python
import functools

import jax
import jax.numpy as jnp
from jax import lax
from jax.experimental import pallas as pl
from jax.experimental.pallas import tpu as pltpu
from jax.sharding import PartitionSpec as P

epsilon = 1e-06
MESH = pl.DeviceIdType.MESH
f32 = jnp.float32
bf16 = jnp.bfloat16
CHUNKS = 4


def dot(a, b):
    return jnp.dot(a, b, preferred_element_type=f32)


def kernel(
    dims,
    outer, inner, values, taps, out_w, tokens, gain, gate_p, up_p, down_p,
    sh_gate, sh_up, sh_down, routes, weights,
    mix_o, exp_o,
    l_outer, l_inner, l_values, halo, prod, l_out_w, l_sg, l_su, l_sd,
    gf, uf, df, nf, og, ld, hid, rt, rv,
    acc, parts, pairs, sums, arrived,
    loc_sem, halo_send, halo_recv, x_send, p_send, t_recv,
    d_send, d_recv, b_send, b_recv, r_send, r_recv, rx_send, rx_recv,
):
    ep, tp, cap = dims
    half = tp // 2
    e, t = lax.axis_index("ep"), lax.axis_index("tp")
    a, b = t // 2, lax.rem(t, 2)
    pair = (e, 2 * a + 1 - b)
    group, ch = l_inner.shape
    rows, width = tokens.shape
    slots = ep * cap
    cols = width // CHUNKS
    n_taps = taps.shape[0]

    def far(d):
        return 2 * lax.rem(a + d, half) + b

    def near(d):
        return 2 * lax.rem(a + half - d, half) + b

    def remote(src, dst, s, r, dev):
        return pltpu.make_async_remote_copy(
            src_ref=src, dst_ref=dst, send_sem=s, recv_sem=r, device_id=dev, device_id_type=MESH
        )

    barrier = pltpu.get_barrier_semaphore()

    def greet(d, _):
        pl.semaphore_signal(barrier, inc=1, device_id=(lax.rem(e + d, ep), t), device_id_type=MESH)
        return 0

    lax.fori_loop(1, ep, greet, 0)
    pl.semaphore_signal(barrier, inc=1, device_id=pair, device_id_type=MESH)
    for d in range(1, half):
        pl.semaphore_signal(barrier, inc=1, device_id=(e, far(d)), device_id_type=MESH)

    local = [
        pltpu.make_async_copy(s, d, loc_sem.at[i])
        for i, (s, d) in enumerate(
            (
                (inner, l_inner), (values, l_values), (outer, l_outer), (out_w, l_out_w),
                (sh_gate, l_sg), (sh_up, l_su), (sh_down, l_sd),
                (gate_p.at[0], gf.at[t]), (up_p.at[0], uf.at[t]), (down_p.at[0], df.at[t]),
            )
        )
    ]
    for c in local:
        c.start()

    pl.semaphore_wait(barrier, ep - 1 + 1 + half - 1)

    kinds = CHUNKS + 3
    n_kind = kinds - 1

    def land(k, s):
        if k == 0:
            return gf.at[s]
        if k == 1:
            return uf.at[s]
        if k == n_kind:
            return nf.at[s]
        return df.at[s, :, pl.ds((k - 2) * cols, cols)]

    def origin(k):
        if k == 0:
            return gate_p.at[0]
        if k == 1:
            return up_p.at[0]
        if k == n_kind:
            return nf.at[t]
        return down_p.at[0, :, pl.ds((k - 2) * cols, cols)]

    def x_copy(k, d):
        return remote(origin(k), land(k, t), x_send.at[k, d], t_recv.at[k, d], (e, far(d)))

    def pair_copy(k):
        return remote(origin(k), land(k, t), p_send.at[k, 0], t_recv.at[k, 0], pair)

    def forward_copy(k, d):
        s = near(d)
        return remote(land(k, s), land(k, s), p_send.at[k, d], t_recv.at[k, half - 1 + d], pair)

    def start_x(k):
        for d in range(1, half):
            x_copy(k, d).start()

    def forward(k):
        for d in range(1, half):
            x_copy(k, d).wait_recv()
            forward_copy(k, d).start()

    def wait_forwarded(k):
        for d in range(1, half):
            forward_copy(k, d).wait_recv()

    for k in range(4):
        start_x(k)
    mine = pl.ds(pl.multiple_of(t * rows, rows), rows)
    own_routes, own_w = routes[:, mine], weights[:, mine]
    slot = lax.broadcasted_iota(jnp.int32, (slots, rows), 0)
    expert = slot // cap
    place = (slot - expert * cap).astype(f32)
    hit = jnp.zeros((slots, rows), f32)
    for k in range(own_routes.shape[0]):
        hit = jnp.where(own_routes[k : k + 1, :] == expert, 1.0, hit)
    upper = lax.broadcasted_iota(jnp.int32, (rows, rows), 0) < lax.broadcasted_iota(
        jnp.int32, (rows, rows), 1
    )
    earlier = dot(hit.astype(bf16), jnp.where(upper, 1.0, 0.0).astype(bf16))
    chosen = jnp.where(earlier == place, hit, 0.0)
    sender = chosen.astype(bf16)

    scales = gain[...].astype(f32).reshape(1, width)

    def norm_rows(i, _):
        at = pl.ds(pl.multiple_of(i * 16, 16), 16)
        v = tokens[at, :].astype(f32)
        square = jnp.mean(v * v, axis=-1, keepdims=True)
        nf[t, at, :] = (v * lax.rsqrt(square + epsilon) * scales).astype(bf16)
        return 0

    lax.fori_loop(0, rows // 16, norm_rows, 0)

    def block(i):
        return pl.ds(pl.multiple_of(i * cap, cap), cap)

    def dispatch_copy(c, d):
        to = lax.rem(e + d, ep)
        at = pl.ds(c * cols, cols)
        return remote(
            og.at[block(to), at], ld.at[block(e), at], d_send.at[c, d], d_recv.at[c, d], (to, t)
        )

    for c in range(CHUNKS):
        at = pl.ds(c * cols, cols)
        og[:, at] = dot(sender, nf[t, :, at]).astype(bf16)

        def start_dispatch(d, _):
            dispatch_copy(c, d).start()
            return 0

        lax.fori_loop(1, ep, start_dispatch, 0)
        ld[block(e), at] = og[block(e), at]
    start_x(n_kind)
    for k in range(kinds):
        pair_copy(k).start()
    for k in range(4, n_kind):
        start_x(k)
    edge = pl.ds(group - 16, 16)
    halos = [
        remote(src.at[edge, :], halo.at[i], halo_send.at[i], halo_recv.at[i], (lax.rem(e + 1, ep), t))
        for i, src in enumerate((inner, values))
    ]
    for c in halos:
        c.start()


    def pair_sum(j, i):
        return remote(
            parts.at[j, 2 * i + 1 - b], pairs.at[j, i], r_send.at[j, i], r_recv.at[j, i], pair
        )

    def far_sum(j, d):
        return remote(
            sums.at[j, d - 1], arrived.at[j, d - 1], rx_send.at[j, d], rx_recv.at[j, d], (e, far(d))
        )

    def start_far(j):
        for d in range(1, half):
            i = lax.rem(a + d, half)
            pair_sum(j, i).wait_recv()
            for c in range(CHUNKS):
                at = pl.ds(c * cols, cols)
                total = parts[j, 2 * i + b, :, at].astype(f32) + pairs[j, i, :, at].astype(f32)
                sums[j, d - 1, :, at] = total.astype(bf16)
            far_sum(j, d).start()

    def finish_sum(j):
        pair_sum(j, a).wait_recv()
        for d in range(1, half):
            far_sum(j, d).wait_recv()

    def summed(j, at):
        total = parts[j, t, :, at].astype(f32) + pairs[j, a, :, at].astype(f32)
        for d in range(1, half):
            total = total + arrived[j, d - 1, :, at].astype(f32)
        return total

    for c in local[:4]:
        c.wait()
    for c in halos:
        c.wait_recv()
    before = halo[0].astype(f32) * halo[1].astype(f32)
    prod[0:16, :] = jnp.where(e > 0, before, 0.0)
    prod[16:, :] = l_inner[...].astype(f32) * l_values[...].astype(f32)
    tap = taps[...].astype(f32)
    for s in range(tp):
        lo = s * rows
        conv = jnp.zeros((rows, ch), f32)
        for j in range(n_taps):
            first = 16 + lo - (n_taps - 1) + j
            conv = conv + tap[j : j + 1, :] * prod[first : first + rows, :]
        gated = (l_outer[lo : lo + rows, :].astype(f32) * conv).astype(bf16)
        for c in range(CHUNKS):
            at = pl.ds(c * cols, cols)
            parts[0, s, :, at] = dot(gated, l_out_w[:, at]).astype(bf16)
    for i in range(half):
        pair_sum(0, i).start()

    for c in local[4:]:
        c.wait()

    def shared(s):
        x = nf[s]
        g = dot(x, l_sg[...])
        u = dot(x, l_su[...])
        h = (g / (1.0 + jnp.exp(-g)) * u).astype(bf16)
        for c in range(CHUNKS):
            at = pl.ds(c * cols, cols)
            parts[1, s, :, at] = dot(h, l_sd[:, at]).astype(bf16)

    shared(t)
    pair_copy(n_kind).wait_recv()
    shared(2 * a + 1 - b)
    pair_sum(1, a).start()

    def act(s, g, u):
        hid[s] = (g / (1.0 + jnp.exp(-g)) * u).astype(bf16)

    pair_copy(0).wait_recv()
    pair_copy(1).wait_recv()
    close = (t, 2 * a + 1 - b)
    for c in range(CHUNKS):
        at = pl.ds(c * cols, cols)

        def wait_dispatch(d, _):
            dispatch_copy(c, d).wait_recv()
            return 0

        lax.fori_loop(1, ep, wait_dispatch, 0)
        for i, s in enumerate(close):
            g, u = dot(ld[:, at], gf[s, at, :]), dot(ld[:, at], uf[s, at, :])
            if c:
                g, u = g + acc[i, 0], u + acc[i, 1]
            if c < CHUNKS - 1:
                acc[i, 0] = g
                acc[i, 1] = u
            else:
                act(s, g, u)
        if c == 1:
            forward(0)
    wait_forwarded(0)
    rest = [near(d) for d in range(1, half)] + [near(d) + 1 - 2 * b for d in range(1, half)]
    gates = [dot(ld[...], gf[s]) for s in rest]
    forward(1)
    for n, s in enumerate(rest):
        if n == half - 1:
            wait_forwarded(1)
        act(s, gates[n], dot(ld[...], uf[s]))

    def back_copy(c, d):
        to = lax.rem(e + d, ep)
        at = pl.ds(c * cols, cols)
        return remote(
            rt.at[block(to), at], rv.at[block(e), at], b_send.at[c, d], b_recv.at[c, d], (to, t)
        )

    for c in range(CHUNKS):
        k = 2 + c
        at = pl.ds(c * cols, cols)
        pair_copy(k).wait_recv()
        forward(k)
        wait_forwarded(k)
        total = dot(hid[0], df[0, :, at])
        for s in range(1, tp):
            total = total + dot(hid[s], df[s, :, at])
        rt[:, at] = total.astype(bf16)

        def start_back(d, _):
            back_copy(c, d).start()
            return 0

        lax.fori_loop(1, ep, start_back, 0)
        rv[block(e), at] = rt[block(e), at]
        if c == 1:
            forward(n_kind)
            for d in range(1, half):
                shared(near(d))
            wait_forwarded(n_kind)
            for d in range(1, half):
                shared(near(d) + 1 - 2 * b)
                pair_sum(1, lax.rem(a + half - d, half)).start()
            start_far(1)
            start_far(0)

    scale = jnp.zeros((slots, rows), f32)
    for k in range(own_routes.shape[0]):
        scale = jnp.where(own_routes[k : k + 1, :] == expert, own_w[k : k + 1, :], scale)
    w_all = jnp.transpose(chosen * scale)
    w_hi = w_all.astype(bf16)
    w_lo = (w_all - w_hi.astype(f32)).astype(bf16)
    finish_sum(1)
    for c in range(CHUNKS):
        at = pl.ds(c * cols, cols)

        def wait_back(d, _):
            back_copy(c, d).wait_recv()
            return 0

        lax.fori_loop(1, ep, wait_back, 0)
        routed = dot(w_hi, rv[:, at]) + dot(w_lo, rv[:, at])
        exp_o[:, at] = (summed(1, at) + routed).astype(bf16)

    finish_sum(0)
    for c in range(CHUNKS):
        at = pl.ds(c * cols, cols)
        mix_o[:, at] = summed(0, at).astype(bf16)
    def sent(d, _):
        for c in range(CHUNKS):
            dispatch_copy(c, d).wait_send()
            back_copy(c, d).wait_send()
        return 0

    lax.fori_loop(1, ep, sent, 0)
    for c in halos:
        c.wait_send()
    for k in range(kinds):
        pair_copy(k).wait_send()
        for d in range(1, half):
            x_copy(k, d).wait_send()
            forward_copy(k, d).wait_send()
    for j in range(2):
        for i in range(half):
            pair_sum(j, i).wait_send()
        for d in range(1, half):
            far_sum(j, d).wait_send()


def per_device(
    outer_gate, inner_gate, conv_values, conv_taps, out_weight, moe_input, norm_gain,
    gate_proj, up_proj, down_proj, shared_gate, shared_up, shared_down, routes, route_weight,
):
    tp = lax.axis_size("tp")
    ep = lax.axis_size("ep")
    half = tp // 2
    group, ch = inner_gate.shape
    rows, width = moe_input.shape
    units = gate_proj.shape[2]
    sh_units = shared_gate.shape[1]
    cap = 2 * rows * routes.shape[1] // ep
    cap = -(-cap // 16) * 16
    slots = ep * cap
    kinds = CHUNKS + 3
    any_spec = pl.BlockSpec(memory_space=pl.ANY)
    vmem = pl.BlockSpec(memory_space=pltpu.VMEM)
    dma = pltpu.SemaphoreType.DMA

    def buf(*shape):
        return pltpu.VMEM(shape, bf16)

    scratch = [
        buf(group, ch), buf(group, ch), buf(group, ch), buf(2, 16, ch),
        pltpu.VMEM((group + 16, ch), f32), buf(ch, width),
        buf(width, sh_units), buf(width, sh_units), buf(sh_units, width),
        buf(tp, width, units), buf(tp, width, units), buf(tp, units, width),
        buf(tp, rows, width), buf(slots, width), buf(slots, width),
        buf(tp, slots, units), buf(slots, width), buf(slots, width),
        pltpu.VMEM((2, 2, slots, units), f32), buf(2, tp, rows, width), buf(2, half, rows, width),
        buf(2, half - 1, rows, width), buf(2, half - 1, rows, width),
        dma((10,)), dma((2,)), dma((2,)), dma((kinds, half)), dma((kinds, half)),
        dma((kinds, tp)), dma((CHUNKS, ep)), dma((CHUNKS, ep)), dma((CHUNKS, ep)), dma((CHUNKS, ep)),
        dma((2, half)), dma((2, half)), dma((2, half)), dma((2, half)),
    ]
    out = pltpu.VMEM((rows, width), bf16)
    return pl.pallas_call(
        functools.partial(kernel, (ep, tp, cap)),
        out_shape=(out, out),
        in_specs=[
            any_spec, any_spec, any_spec, vmem, any_spec, vmem, vmem,
            any_spec, any_spec, any_spec, any_spec, any_spec, any_spec, vmem, vmem,
        ],
        out_specs=(vmem, vmem),
        scratch_shapes=scratch,
        compiler_params=pltpu.CompilerParams(
            collective_id=0, has_side_effects=True, vmem_limit_bytes=65536000
        ),
    )(
        outer_gate, inner_gate, conv_values, conv_taps, out_weight, moe_input,
        norm_gain, gate_proj, up_proj, down_proj,
        shared_gate, shared_up, shared_down, routes.T, route_weight.T,
    )


def solution(mesh):
    return jax.shard_map(
        per_device,
        mesh=mesh,
        in_specs=(
            P("ep", "tp"), P("ep", "tp"), P("ep", "tp"), P(None, "tp"), P("tp", None),
            P(("ep", "tp"), None), P(),
            P("ep", None, "tp"), P("ep", None, "tp"), P("ep", "tp", None),
            P(None, "tp"), P(None, "tp"), P("tp", None), P("ep", None), P("ep", None),
        ),
        out_specs=(P(("ep", "tp"), None), P(("ep", "tp"), None)),
        check_vma=False,
    )
```
